32 devices in a mesh: dp: 4 (over y, x), kv: 4 (over z), tp: 2 (over core).
Axes of the slice: x: 2, y: 2, z: 4, core: 2. Of those that a mesh axis runs over, the one named last changes fastest.
Arguments:
- tokens: bfloat16 [32, 4096], P('dp', ('kv', 'tp')), may hold values from -7 to 7
- mix_gain: float32 [4096], replicated, may hold values from 0.1 to 1.9
- query_weight: bfloat16 [16, 128, 4096], P('tp', 'kv'), may hold values from -0.09375 to 0.09375
- forget_weight: bfloat16 [16, 128, 4096], P('tp', 'kv'), may hold values from -0.09375 to 0.09375
- value_weight: bfloat16 [16, 128, 4096], P('tp', 'kv'), may hold values from -0.09375 to 0.09375
- gate_weight: bfloat16 [16, 128, 4096], P('tp', 'kv'), may hold values from -0.09375 to 0.09375
- lower_bound: float32 [16, 128], P('tp'), may hold values from 0.02 to 0.9
- recurrent_state: float32 [32, 16, 128, 128], P(('dp', 'kv'), 'tp'), may hold values from -3 to 3
- head_gain: float32 [16, 128], P('tp'), may hold values from 0.1 to 1.9
- out_weight: bfloat16 [16, 128, 4096], P(None, None, ('kv', 'tp')), may hold values from -0.125 to 0.125
- mlp_gain: float32 [4096], replicated, may hold values from 0.1 to 1.9
- up_weight: bfloat16 [4096, 16384], P(None, ('kv', 'tp')), may hold values from -0.09375 to 0.09375
- down_weight: bfloat16 [16384, 4096], P(('kv', 'tp')), may hold values from -0.0625 to 0.0625
Outputs:
- layer_output: bfloat16 [32, 4096], P('dp', ('kv', 'tp'))
- next_state: float32 [32, 16, 128, 128], P(('dp', 'kv'), 'tp')
The draws below stay inside these ranges and needn't reach their ends.
All inputs are finite; a program needn't handle non-finite values.
Results may differ from the reference program's by a relative error of at most 0.0072.
Values may be sent and summed in bfloat16 or wider, within the bound.
A program may use at most 128 MiB of HBM per device.

```python
import math
import jax
import jax.numpy as jnp
from jax import lax

D = 4096
HEADS = 16
KEY_DIM = 128
VALUE_DIM = 128
FF = 16384
BATCH = 32


def draw_tokens(key, part):
    noise_key = jax.random.fold_in(jax.random.fold_in(key, 17), 0)
    column = jnp.arange(D, dtype=jnp.float32) / (D - 1)
    values = jnp.clip(jax.random.normal(noise_key, (BATCH, D), jnp.float32), -4.0, 4.0)
    spread = math.log(3.0)
    scaled = values * jnp.exp(spread * (column - 0.5))
    return scaled.astype(jnp.bfloat16)


def raised(entries, own_key, source, target, shards_of, factor):
    def block_of(axis_at):
        return (jnp.arange(entries.shape[axis_at]) // (entries.shape[axis_at] // shards_of)).reshape((-1,) + (1,) * (entries.ndim - 1 - axis_at))

    first = jax.random.permutation(own_key, shards_of)[block_of(target)]
    other_side = (block_of(target) + shards_of // 2) % shards_of
    return jnp.where((block_of(source) == first) | (block_of(source) == other_side), factor * entries, entries)


def level_of(own_key, extent, pieces, low, largest):
    loudness = 1.0
    for dim, shards_of in pieces:
        draws = jax.random.uniform(jax.random.fold_in(jax.random.fold_in(own_key, 6), dim), (shards_of,), jnp.float32, low / len(pieces), largest / len(pieces))
        loudness = loudness * jnp.repeat(jnp.exp(draws), extent[dim] // shards_of).reshape((-1,) + (1,) * (len(extent) - 1 - dim))
    return loudness


def centred(own_key, dims, deviation, limit, cuts=(), kind=jnp.bfloat16):
    level = level_of(own_key, dims, cuts, -0.22, 0.18) if cuts else 1.0
    drawn = jax.random.normal(own_key, dims, jnp.float32) * deviation * level
    return jnp.minimum(jnp.maximum(drawn, -limit), limit).astype(kind)


def gaussian_with(stream_key, dims, deviation, bound, pieces, heavy, held_as=jnp.bfloat16):
    drawn = deviation * jax.random.normal(stream_key, dims, jnp.float32)
    if pieces:
        drawn = drawn * level_of(stream_key, dims, pieces, -0.22, 0.18)
    return jnp.clip(raised(drawn, jax.random.fold_in(stream_key, 3), *heavy), -bound, bound).astype(held_as)


def setup_inputs(seed: int = 0) -> dict:
    key_of = jax.random.split(jax.random.key(seed), 14)
    return {
        "tokens": draw_tokens(jax.random.fold_in(key_of[13], 71), 0),
        "mix_gain": jnp.clip(1.0 + 0.18 * jax.random.normal(key_of[1], (D,), jnp.float32), 0.1, 1.9),
        "query_weight": centred(key_of[2], (HEADS, KEY_DIM, D), D ** -0.5, 0.09375, ((0, 2), (1, 4))),
        "forget_weight": centred(key_of[3], (HEADS, KEY_DIM, D), D ** -0.5, 0.09375, ((0, 2), (1, 4))),
        "value_weight": centred(key_of[4], (HEADS, VALUE_DIM, D), D ** -0.5, 0.09375, ((0, 2), (1, 4))),
        "gate_weight": centred(key_of[5], (HEADS, VALUE_DIM, D), D ** -0.5, 0.09375, ((0, 2), (1, 4))),
        "lower_bound": jnp.clip(jnp.exp(math.log(0.9) - 3.8066625 * jax.random.uniform(key_of[6], (HEADS, KEY_DIM), jnp.float32) ** level_of(key_of[6], (HEADS, KEY_DIM), ((0, 2),), -0.2, 0.2)), 0.02, 0.9),
        "recurrent_state": centred(key_of[7], (BATCH, HEADS, KEY_DIM, VALUE_DIM), 0.5, 3.0, ((0, 16), (1, 2)), jnp.float32),
        "head_gain": jnp.clip(1.0 + 0.18 * jax.random.normal(key_of[8], (HEADS, VALUE_DIM), jnp.float32), 0.1, 1.9),
        "out_weight": centred(key_of[9], (HEADS, VALUE_DIM, D), (HEADS * VALUE_DIM) ** -0.5, 0.125, ((2, 8),)),
        "mlp_gain": jnp.clip(1.0 + 0.18 * jax.random.normal(key_of[10], (D,), jnp.float32), 0.1, 1.9),
        "up_weight": centred(key_of[11], (D, FF), D ** -0.5, 0.09375, ((1, 8),)),
        "down_weight": gaussian_with(key_of[12], (FF, D), FF ** -0.5, 0.0625, ((0, 8),), (0, 1, 8, 2.0)),
    }


epsilon = 1e-06

def rms_rows(matrix, gain_vector):
    as_float = matrix.astype(jnp.float32)
    inv_root = lax.rsqrt(lax.optimization_barrier(jnp.mean(as_float * as_float, axis=1, keepdims=True)) + epsilon)
    return (as_float * inv_root * gain_vector).astype(jnp.bfloat16)

def project_rows(normed, weight):
    flat_weight = weight.reshape(-1, weight.shape[2])
    product = lax.dot_general(normed, flat_weight, (((1,), (1,)), ((), ())), preferred_element_type=jnp.float32).astype(jnp.bfloat16)
    return product.reshape(normed.shape[0], weight.shape[0], weight.shape[1])

def reference(tokens, mix_gain, query_weight, forget_weight, value_weight, gate_weight, lower_bound, recurrent_state, head_gain, out_weight, mlp_gain, up_weight, down_weight):
    normed = rms_rows(tokens, mix_gain)
    pre_query, pre_forget, value_rows, pre_gate = lax.optimization_barrier((project_rows(normed, query_weight), project_rows(normed, forget_weight), project_rows(normed, value_weight), project_rows(normed, gate_weight)))
    log_forget = jnp.logaddexp(jnp.log(lower_bound), jnp.log1p(-lower_bound) + jax.nn.log_sigmoid(pre_forget.astype(jnp.float32)))
    key_rows = -jnp.expm1(log_forget)
    next_state = jnp.exp(log_forget)[:, :, :, None] * recurrent_state + key_rows[:, :, :, None] * value_rows.astype(jnp.float32)[:, :, None, :]
    query_act = jax.nn.silu(pre_query.astype(jnp.float32))
    readout = jnp.einsum('bhk,bhkv->bhv', query_act, next_state, precision=lax.Precision.HIGHEST)
    inv_head = lax.rsqrt(lax.optimization_barrier(jnp.mean(readout * readout, axis=2, keepdims=True)) + epsilon)
    mixed_heads = (readout * inv_head * head_gain * jax.nn.silu(pre_gate.astype(jnp.float32))).astype(jnp.bfloat16)
    projected = jnp.dot(mixed_heads.reshape(mixed_heads.shape[0], -1), out_weight.reshape(-1, out_weight.shape[2]), preferred_element_type=jnp.float32)
    residual = lax.optimization_barrier((tokens.astype(jnp.float32) + projected).astype(jnp.bfloat16))
    normed_mlp = rms_rows(residual, mlp_gain)
    hidden = jnp.square(jax.nn.relu(jnp.dot(normed_mlp, up_weight, preferred_element_type=jnp.float32))).astype(jnp.bfloat16)
    layer_output = (residual.astype(jnp.float32) + jnp.dot(hidden, down_weight, preferred_element_type=jnp.float32)).astype(jnp.bfloat16)
    return (layer_output, next_state)
```

```python
import functools

import jax
import jax.numpy as jnp
from jax import lax
from jax.experimental import pallas as pl
from jax.experimental.pallas import tpu as pltpu
from jax.sharding import PartitionSpec as P

epsilon = 1e-06
VMEM_LIMIT = 67043328
MESH = pl.DeviceIdType.MESH


def normed_rows(row_block, gain_vector):
    whole_rows = lax.all_gather(row_block, ("kv", "tp"), axis=1, tiled=True).astype(jnp.float32)
    inv_root = lax.rsqrt(jnp.mean(whole_rows * whole_rows, axis=1, keepdims=True) + epsilon)
    result_rows = (whole_rows * inv_root * gain_vector).astype(jnp.bfloat16)
    return result_rows


def local_plain(
    tokens,
    mix_gain,
    query_weight,
    forget_weight,
    value_weight,
    gate_weight,
    lower_bound,
    recurrent_state,
    head_gain,
    out_weight,
    mlp_gain,
    up_weight,
    down_weight,
):
    normed = normed_rows(tokens, mix_gain)
    local_heads, local_chan, width = query_weight.shape
    stacked = jnp.stack((query_weight, forget_weight, value_weight, gate_weight), axis=0).reshape(
        -1, width
    )
    product = lax.dot_general(
        normed, stacked, (((1,), (1,)), ((), ())), preferred_element_type=jnp.float32
    ).astype(jnp.bfloat16)
    product = product.reshape(normed.shape[0], 4, local_heads, local_chan)
    pre_query, pre_forget, value_rows, pre_gate = (
        lax.all_to_all(product[:, 0], "kv", split_axis=0, concat_axis=2, tiled=True),
        lax.all_to_all(product[:, 1], "kv", split_axis=0, concat_axis=2, tiled=True),
        lax.all_to_all(product[:, 2], "kv", split_axis=0, concat_axis=2, tiled=True),
        lax.all_to_all(product[:, 3], "kv", split_axis=0, concat_axis=2, tiled=True),
    )
    log_forget = jnp.logaddexp(
        jnp.log(lower_bound),
        jnp.log1p(-lower_bound) + jax.nn.log_sigmoid(pre_forget.astype(jnp.float32)),
    )
    key_rows = -jnp.expm1(log_forget)
    next_state = (
        jnp.exp(log_forget)[:, :, :, None] * recurrent_state
        + key_rows[:, :, :, None] * value_rows.astype(jnp.float32)[:, :, None, :]
    )
    query_act = jax.nn.silu(pre_query.astype(jnp.float32))
    readout = jnp.einsum("bhk,bhkv->bhv", query_act, next_state, precision=lax.Precision.HIGHEST)
    inv_head = lax.rsqrt(jnp.mean(readout * readout, axis=2, keepdims=True) + epsilon)
    mixed_heads = (
        readout * inv_head * head_gain * jax.nn.silu(pre_gate.astype(jnp.float32))
    ).astype(jnp.bfloat16)
    all_heads = lax.all_gather(mixed_heads, "tp", axis=1, tiled=True)
    flat_mixed = all_heads.reshape(all_heads.shape[0], -1)
    out_matrix = out_weight.reshape(-1, out_weight.shape[2])
    projected = jnp.dot(
        lax.all_gather(flat_mixed, "kv", axis=0, tiled=True),
        out_matrix,
        preferred_element_type=jnp.float32,
    )
    residual = lax.optimization_barrier(
        (tokens.astype(jnp.float32) + projected).astype(jnp.bfloat16)
    )
    normed_mlp = normed_rows(residual, mlp_gain)
    hidden = jnp.square(
        jax.nn.relu(jnp.dot(normed_mlp, up_weight, preferred_element_type=jnp.float32))
    ).astype(jnp.bfloat16)
    summed = lax.psum_scatter(
        jnp.dot(hidden, down_weight, preferred_element_type=jnp.float32),
        ("kv", "tp"),
        scatter_dimension=1,
        tiled=True,
    )
    layer_output = (residual.astype(jnp.float32) + summed).astype(jnp.bfloat16)
    return (layer_output, next_state)


def sigmoid(x):
    return 1.0 / (1.0 + jnp.exp(-x))


def kernel(
    KV, TP, LH, UP_CHUNKS, DOWN_CHUNKS,
    tok_h, mixg_h, qw_h, fw_h, vw_h, gw_h, lb_h, st_h, hg_h, ow_h, mlpg_h, uw_h, dw_h,
    out_h, ns_h,
    xsrc, mixg, lb, hg, mlpg, wbuf, stbuf, nsbuf, obuf, ubuf, dbuf, outbuf,
    xbuf, asend, arecv, heads, msend, mrecv, rsend, rbuf, psend, pbuf, xn, hid,
    local_sem, up_sem, down_sem, send_sem, recv_sem,
):
    N = KV * TP
    kv, tp = lax.axis_index("kv"), lax.axis_index("tp")
    me = kv * TP + tp
    nb, block = xsrc.shape
    per = stbuf.shape[0] // LH
    lane = stbuf.shape[2]
    lc = wbuf.shape[1] // LH

    small = [
        pltpu.make_async_copy(src, dst, local_sem.at[i])
        for i, (src, dst) in enumerate(
            ((tok_h, xsrc), (mixg_h, mixg), (lb_h, lb), (hg_h, hg), (mlpg_h, mlpg))
        )
    ]
    weights = [
        pltpu.make_async_copy(src, wbuf.at[i], local_sem.at[5 + i])
        for i, src in enumerate((qw_h, fw_h, vw_h, gw_h))
    ]
    state_in = pltpu.make_async_copy(st_h, stbuf, local_sem.at[9])
    out_in = pltpu.make_async_copy(ow_h, obuf, local_sem.at[10])
    uk = ubuf.shape[0] // UP_CHUNKS
    ups = [
        pltpu.make_async_copy(
            uw_h.at[pl.ds(i * uk, uk)], ubuf.at[pl.ds(i * uk, uk)], up_sem.at[i]
        )
        for i in range(UP_CHUNKS)
    ]
    dk = dbuf.shape[0] // DOWN_CHUNKS
    downs = [
        pltpu.make_async_copy(
            dw_h.at[pl.ds(i * dk, dk)], dbuf.at[pl.ds(i * dk, dk)], down_sem.at[i]
        )
        for i in range(DOWN_CHUNKS)
    ]
    for copy in small + weights + [state_in, out_in] + ups + downs:
        copy.start()

    def where(index):
        return {"kv": index // TP, "tp": lax.rem(index, TP)}

    barrier = pltpu.get_barrier_semaphore()
    for o in range(1, N):
        pl.semaphore_signal(
            barrier, inc=1, device_id=where(lax.rem(me + o, N)), device_id_type=MESH
        )
    pl.semaphore_wait(barrier, N - 1)

    def push(phase, src, dst, o, peer):
        copy = pltpu.make_async_remote_copy(
            src_ref=src,
            dst_ref=dst,
            send_sem=send_sem.at[phase, o],
            recv_sem=recv_sem.at[phase, me],
            device_id=where(peer),
            device_id_type=MESH,
        )
        copy.start()
        return copy

    def take(phase, src, dst, peer):
        pltpu.make_async_remote_copy(
            src_ref=src,
            dst_ref=dst,
            send_sem=send_sem.at[phase, 0],
            recv_sem=recv_sem.at[phase, peer],
            device_id=where(peer),
            device_id_type=MESH,
        ).wait_recv()

    sent = []

    def gather(phase, src, buf):
        for o in range(1, N):
            sent.append(push(phase, src, buf.at[me], o, lax.rem(me + o, N)))
        buf[me] = src[...]
        for o in range(1, N):
            peer = lax.rem(me + o, N)
            take(phase, src, buf.at[peer], peer)

    def norm_into(buf, gain):
        total = jnp.zeros((nb, 1), jnp.float32)
        for j in range(N):
            piece = buf[j].astype(jnp.float32)
            total = total + jnp.sum(piece * piece, axis=1, keepdims=True)
        inv = lax.rsqrt(total / (N * block) + epsilon)
        for j in range(N):
            cols = slice(j * block, (j + 1) * block)
            piece = buf[j].astype(jnp.float32)
            xn[:, cols] = (piece * inv * gain[:, cols]).astype(jnp.bfloat16)

    small[0].wait()
    gather(0, xsrc, xbuf)
    small[1].wait()
    norm_into(xbuf, mixg)

    for w in range(4):
        weights[w].wait()
        prod = lax.dot_general(
            xn[...], wbuf[w], (((1,), (1,)), ((), ())), preferred_element_type=jnp.float32
        )
        prod = prod.astype(jnp.bfloat16).astype(jnp.float32)
        for j in range(KV):
            asend[j, w * per : (w + 1) * per, :] = prod[j * per : (j + 1) * per, :]
    for o in range(1, KV):
        other = lax.rem(kv + o, KV)
        sent.append(push(1, asend.at[other], arecv.at[kv], o, other * TP + tp))
    arecv[kv] = asend[kv]
    for copy in small[2:]:
        copy.wait()
    for o in range(1, KV):
        other = lax.rem(kv + o, KV)
        take(1, asend.at[other], arecv.at[other], other * TP + tp)
    for h in range(LH):
        row = jnp.concatenate(
            [arecv[s, :, h * lc : (h + 1) * lc] for s in range(KV)], axis=1
        )
        for i in range(4 * per):
            heads[i, h : h + 1, :] = row[i : i + 1, :]

    def kind(w):
        return heads[w * per : (w + 1) * per].reshape(per * LH, lane)

    low = jnp.concatenate([lb[...]] * per, axis=0)
    pre_q, pre_f, val, gate = kind(0), kind(1), kind(2), kind(3)
    forget = low + (1.0 - low) * sigmoid(pre_f)
    key = (1.0 - low) * sigmoid(-pre_f)
    query = pre_q * sigmoid(pre_q)
    items = per * LH
    stacked = jnp.concatenate(
        [forget, key, query, jnp.zeros((lane - 3 * items, lane), jnp.float32)], axis=0
    )
    cols = stacked.T
    state_in.wait()
    rows = []
    for i in range(items):
        new = (
            cols[:, i : i + 1] * stbuf[i]
            + cols[:, items + i : items + i + 1] * val[i : i + 1, :]
        )
        nsbuf[i] = new
        rows.append(
            jnp.sum(cols[:, 2 * items + i : 2 * items + i + 1] * new, axis=0, keepdims=True)
        )
    readout = jnp.concatenate(rows, axis=0)
    state_out = pltpu.make_async_copy(nsbuf, ns_h, local_sem.at[11])
    state_out.start()
    inv_head = lax.rsqrt(jnp.mean(readout * readout, axis=1, keepdims=True) + epsilon)
    gains = jnp.concatenate([hg[...]] * per, axis=0)
    mixed = readout * inv_head * gains * (gate * sigmoid(gate))
    for r in range(per):
        for h in range(LH):
            msend[r : r + 1, h * lane : (h + 1) * lane] = mixed[r * LH + h : r * LH + h + 1, :]
    gather(2, msend, mrecv)
    flat = jnp.concatenate(
        [
            jnp.concatenate([mrecv[s * TP + t] for s in range(KV)], axis=0)
            for t in range(TP)
        ],
        axis=1,
    ).astype(jnp.bfloat16)

    out_in.wait()
    projected = jnp.dot(flat, obuf[...], preferred_element_type=jnp.float32)
    rsend[...] = (xsrc[...].astype(jnp.float32) + projected).astype(jnp.bfloat16)
    gather(3, rsend, rbuf)
    norm_into(rbuf, mlpg)

    for copy in ups:
        copy.wait()
    tile = min(512, ubuf.shape[1])

    @pl.loop(0, ubuf.shape[1] // tile)
    def _(n):
        at = pl.ds(pl.multiple_of(n * tile, tile), tile)
        act = jnp.maximum(jnp.dot(xn[...], ubuf[:, at], preferred_element_type=jnp.float32), 0.0)
        hid[:, at] = (act * act).astype(jnp.bfloat16)

    for copy in downs:
        copy.wait()

    def partial_sum(peer):
        at = pl.ds(pl.multiple_of(peer * block, block), block)
        return jnp.dot(hid[...], dbuf[:, at], preferred_element_type=jnp.float32)

    @pl.loop(1, N)
    def _(o):
        peer = lax.rem(me + o, N)
        psend[o] = partial_sum(peer)
        push(4, psend.at[o], pbuf.at[me], o, peer)

    pbuf[me] = partial_sum(me)
    for o in range(1, N):
        peer = lax.rem(me + o, N)
        take(4, psend.at[0], pbuf.at[peer], peer)
    summed = pbuf[0]
    for j in range(1, N):
        summed = summed + pbuf[j]
    outbuf[...] = (rsend[...].astype(jnp.float32) + summed).astype(jnp.bfloat16)
    last = pltpu.make_async_copy(outbuf, out_h, local_sem.at[0])
    last.start()
    for copy in sent:
        copy.wait_send()
    for o in range(1, N):
        pltpu.make_async_remote_copy(
            src_ref=psend.at[o],
            dst_ref=pbuf.at[me],
            send_sem=send_sem.at[4, o],
            recv_sem=recv_sem.at[4, me],
            device_id=where(lax.rem(me + o, N)),
            device_id_type=MESH,
        ).wait_send()
    last.wait()
    state_out.wait()


def local_kernel(KV, TP, *args):
    (tokens, mix_gain, qw, fw, vw, gw, lower_bound, state, head_gain, ow, mlp_gain, uw, dw) = args
    nb, block = tokens.shape
    LH, lc, D = qw.shape
    per, _, kd, vd = state.shape
    N = KV * TP
    UP, DOWN = 8, 8
    bf, f32 = jnp.bfloat16, jnp.float32
    flat = lambda a: a.reshape(-1, a.shape[-1])
    hidden = uw.shape[1]
    out, ns = pl.pallas_call(
        functools.partial(kernel, KV, TP, LH, UP, DOWN),
        out_shape=(
            jax.ShapeDtypeStruct((nb, block), bf),
            jax.ShapeDtypeStruct((per * LH, kd, vd), f32),
        ),
        in_specs=[pl.BlockSpec(memory_space=pl.ANY)] * 13,
        out_specs=(pl.BlockSpec(memory_space=pl.ANY),) * 2,
        scratch_shapes=[
            pltpu.VMEM((nb, block), bf),
            pltpu.VMEM((1, D), f32),
            pltpu.VMEM((LH, kd), f32),
            pltpu.VMEM((LH, vd), f32),
            pltpu.VMEM((1, D), f32),
            pltpu.VMEM((4, LH * lc, D), bf),
            pltpu.VMEM((per * LH, kd, vd), f32),
            pltpu.VMEM((per * LH, kd, vd), f32),
            pltpu.VMEM((ow.shape[0] * ow.shape[1], block), bf),
            pltpu.VMEM(uw.shape, bf),
            pltpu.VMEM(dw.shape, bf),
            pltpu.VMEM((nb, block), bf),
            pltpu.VMEM((N, nb, block), bf),
            pltpu.VMEM((KV, 4 * per, LH * lc), f32),
            pltpu.VMEM((KV, 4 * per, LH * lc), f32),
            pltpu.VMEM((4 * per, LH, kd), f32),
            pltpu.VMEM((per, LH * vd), f32),
            pltpu.VMEM((N, per, LH * vd), f32),
            pltpu.VMEM((nb, block), bf),
            pltpu.VMEM((N, nb, block), bf),
            pltpu.VMEM((N, nb, block), f32),
            pltpu.VMEM((N, nb, block), f32),
            pltpu.VMEM((nb, D), bf),
            pltpu.VMEM((nb, hidden), bf),
            pltpu.SemaphoreType.DMA((12,)),
            pltpu.SemaphoreType.DMA((UP,)),
            pltpu.SemaphoreType.DMA((DOWN,)),
            pltpu.SemaphoreType.DMA((5, N)),
            pltpu.SemaphoreType.DMA((5, N)),
        ],
        compiler_params=pltpu.CompilerParams(
            collective_id=0, has_side_effects=True, vmem_limit_bytes=VMEM_LIMIT
        ),
    )(
        tokens, mix_gain.reshape(1, -1), flat(qw), flat(fw), flat(vw), flat(gw), lower_bound,
        state.reshape(-1, kd, vd), head_gain, flat(ow), mlp_gain.reshape(1, -1), uw, dw,
    )
    return out, ns.reshape(state.shape)


def local(KV, TP, *args):
    tokens, qw, state = args[0], args[2], args[7]
    nb, block = tokens.shape
    LH, lc, _ = qw.shape
    per, _, kd, vd = state.shape
    fits = (
        block % 128 == 0
        and (LH * lc) % 128 == 0
        and kd == 128
        and vd == 128
        and nb % 8 == 0
        and (4 * per) % 8 == 0
        and LH % 8 == 0
        and 3 * per * LH <= kd
        and args[11].shape[1] % 512 == 0
        and KV > 1
    )
    if fits:
        return local_kernel(KV, TP, *args)
    return local_plain(*args)


def solution(mesh):
    placed = (
        P("dp", ("kv", "tp")),
        P(),
        P("tp", "kv", None),
        P("tp", "kv", None),
        P("tp", "kv", None),
        P("tp", "kv", None),
        P("tp", None),
        P(("dp", "kv"), "tp", None, None),
        P("tp", None),
        P(None, None, ("kv", "tp")),
        P(),
        P(None, ("kv", "tp")),
        P(("kv", "tp"), None),
    )
    return jax.shard_map(
        functools.partial(local, mesh.shape["kv"], mesh.shape["tp"]),
        mesh=mesh,
        in_specs=placed,
        out_specs=(P("dp", ("kv", "tp")), P(("dp", "kv"), "tp", None, None)),
        check_vma=False,
    )
```

```python
import functools

import jax
import jax.numpy as jnp
from jax import lax
from jax.experimental import pallas as pl
from jax.experimental.pallas import tpu as pltpu
from jax.sharding import PartitionSpec as P

epsilon = 1e-06
VMEM_LIMIT = 67043328
MESH = pl.DeviceIdType.MESH


def normed_rows(row_block, gain_vector):
    whole_rows = lax.all_gather(row_block, ("kv", "tp"), axis=1, tiled=True).astype(jnp.float32)
    inv_root = lax.rsqrt(jnp.mean(whole_rows * whole_rows, axis=1, keepdims=True) + epsilon)
    result_rows = (whole_rows * inv_root * gain_vector).astype(jnp.bfloat16)
    return result_rows


def local_plain(
    tokens,
    mix_gain,
    query_weight,
    forget_weight,
    value_weight,
    gate_weight,
    lower_bound,
    recurrent_state,
    head_gain,
    out_weight,
    mlp_gain,
    up_weight,
    down_weight,
):
    normed = normed_rows(tokens, mix_gain)
    local_heads, local_chan, width = query_weight.shape
    stacked = jnp.stack((query_weight, forget_weight, value_weight, gate_weight), axis=0).reshape(
        -1, width
    )
    product = lax.dot_general(
        normed, stacked, (((1,), (1,)), ((), ())), preferred_element_type=jnp.float32
    ).astype(jnp.bfloat16)
    product = product.reshape(normed.shape[0], 4, local_heads, local_chan)
    pre_query, pre_forget, value_rows, pre_gate = (
        lax.all_to_all(product[:, 0], "kv", split_axis=0, concat_axis=2, tiled=True),
        lax.all_to_all(product[:, 1], "kv", split_axis=0, concat_axis=2, tiled=True),
        lax.all_to_all(product[:, 2], "kv", split_axis=0, concat_axis=2, tiled=True),
        lax.all_to_all(product[:, 3], "kv", split_axis=0, concat_axis=2, tiled=True),
    )
    log_forget = jnp.logaddexp(
        jnp.log(lower_bound),
        jnp.log1p(-lower_bound) + jax.nn.log_sigmoid(pre_forget.astype(jnp.float32)),
    )
    key_rows = -jnp.expm1(log_forget)
    next_state = (
        jnp.exp(log_forget)[:, :, :, None] * recurrent_state
        + key_rows[:, :, :, None] * value_rows.astype(jnp.float32)[:, :, None, :]
    )
    query_act = jax.nn.silu(pre_query.astype(jnp.float32))
    readout = jnp.einsum("bhk,bhkv->bhv", query_act, next_state, precision=lax.Precision.HIGHEST)
    inv_head = lax.rsqrt(jnp.mean(readout * readout, axis=2, keepdims=True) + epsilon)
    mixed_heads = (
        readout * inv_head * head_gain * jax.nn.silu(pre_gate.astype(jnp.float32))
    ).astype(jnp.bfloat16)
    all_heads = lax.all_gather(mixed_heads, "tp", axis=1, tiled=True)
    flat_mixed = all_heads.reshape(all_heads.shape[0], -1)
    out_matrix = out_weight.reshape(-1, out_weight.shape[2])
    projected = jnp.dot(
        lax.all_gather(flat_mixed, "kv", axis=0, tiled=True),
        out_matrix,
        preferred_element_type=jnp.float32,
    )
    residual = lax.optimization_barrier(
        (tokens.astype(jnp.float32) + projected).astype(jnp.bfloat16)
    )
    normed_mlp = normed_rows(residual, mlp_gain)
    hidden = jnp.square(
        jax.nn.relu(jnp.dot(normed_mlp, up_weight, preferred_element_type=jnp.float32))
    ).astype(jnp.bfloat16)
    summed = lax.psum_scatter(
        jnp.dot(hidden, down_weight, preferred_element_type=jnp.float32),
        ("kv", "tp"),
        scatter_dimension=1,
        tiled=True,
    )
    layer_output = (residual.astype(jnp.float32) + summed).astype(jnp.bfloat16)
    return (layer_output, next_state)


def sigmoid(x):
    return 1.0 / (1.0 + jnp.exp(-x))


def kernel(
    KV, TP, LH, UP_CHUNKS, DOWN_CHUNKS,
    tok_h, mixg_h, qw_h, fw_h, vw_h, gw_h, lb_h, st_h, hg_h, ow_h, mlpg_h, uw_h, dw_h,
    out_h, ns_h,
    xsrc, mixg, lb, hg, mlpg, wbuf, stbuf, nsbuf, obuf, ubuf, dbuf, outbuf,
    xbuf, asend, arecv, heads, mrow, msend, mrecv, rsend, rbuf, psend, pbuf, acc, hid,
    local_sem, up_sem, down_sem, send_sem, recv_sem,
):
    N = KV * TP
    kv, tp = lax.axis_index("kv"), lax.axis_index("tp")
    me = kv * TP + tp
    nb, block = xsrc.shape
    per = stbuf.shape[0] // LH
    lane = stbuf.shape[2]
    lc = wbuf.shape[1] // LH

    small = [
        pltpu.make_async_copy(src, dst, local_sem.at[i])
        for i, (src, dst) in enumerate(
            ((tok_h, xsrc), (mixg_h, mixg), (lb_h, lb), (hg_h, hg), (mlpg_h, mlpg))
        )
    ]
    weights = [
        pltpu.make_async_copy(src, wbuf.at[i], local_sem.at[5 + i])
        for i, src in enumerate((qw_h, fw_h, vw_h, gw_h))
    ]
    state_in = pltpu.make_async_copy(st_h, stbuf, local_sem.at[9])
    out_in = pltpu.make_async_copy(ow_h, obuf, local_sem.at[10])
    uk = ubuf.shape[0] // UP_CHUNKS
    ups = [
        pltpu.make_async_copy(
            uw_h.at[pl.ds(i * uk, uk)], ubuf.at[pl.ds(i * uk, uk)], up_sem.at[i]
        )
        for i in range(UP_CHUNKS)
    ]
    dk = dbuf.shape[0] // DOWN_CHUNKS
    downs = [
        pltpu.make_async_copy(
            dw_h.at[pl.ds(i * dk, dk)], dbuf.at[pl.ds(i * dk, dk)], down_sem.at[i]
        )
        for i in range(DOWN_CHUNKS)
    ]
    for copy in small + weights:
        copy.start()

    def where(index):
        return {"kv": index // TP, "tp": lax.rem(index, TP)}

    barrier = pltpu.get_barrier_semaphore()
    for o in range(1, N):
        pl.semaphore_signal(
            barrier, inc=1, device_id=where(lax.rem(me + o, N)), device_id_type=MESH
        )
    for copy in [state_in, out_in] + ups:
        copy.start()
    pl.semaphore_wait(barrier, N - 1)

    def flip(index, mask):
        bit = 1
        result = index
        while bit <= mask:
            if mask & bit:
                result = result + bit - 2 * bit * lax.rem(index // bit, 2)
            bit *= 2
        return result

    order = [flip(kv, m // TP) * TP + lax.rem(tp + m, TP) for m in range(N)]

    def push(phase, src, dst, o, peer):
        copy = pltpu.make_async_remote_copy(
            src_ref=src,
            dst_ref=dst,
            send_sem=send_sem.at[phase, o],
            recv_sem=recv_sem.at[phase, me],
            device_id=where(peer),
            device_id_type=MESH,
        )
        copy.start()
        return copy

    def take(phase, src, dst, peer):
        pltpu.make_async_remote_copy(
            src_ref=src,
            dst_ref=dst,
            send_sem=send_sem.at[phase, 0],
            recv_sem=recv_sem.at[phase, peer],
            device_id=where(peer),
            device_id_type=MESH,
        ).wait_recv()

    sent = []

    def spread(phase, src, buf):
        for o in reversed(range(1, N)):
            sent.append(push(phase, src, buf.at[me], o, order[o]))
        buf[me] = src[...]

    def columns(peer):
        return pl.ds(pl.multiple_of(peer * block, block), block)

    def scaled(piece, gain, at, total):
        piece = piece.astype(jnp.float32)
        total = total + jnp.sum(piece * piece, axis=1, keepdims=True)
        return (piece * gain[:, at]).astype(jnp.bfloat16), total

    def inverse(total):
        return lax.rsqrt(total / (N * block) + epsilon)

    small[0].wait()
    spread(0, xsrc, xbuf)
    small[1].wait()
    for copy in weights:
        copy.wait()
    for copy in downs:
        copy.start()
    total = jnp.zeros((nb, 1), jnp.float32)
    prods = [jnp.zeros((nb, wbuf.shape[1]), jnp.float32)] * 4
    for o in range(N):
        peer = order[o]
        if o:
            take(0, xsrc, xbuf.at[peer], peer)
        at = columns(peer)
        piece, total = scaled(xbuf[peer], mixg, at, total)
        for w in range(4):
            prods[w] = prods[w] + lax.dot_general(
                piece,
                wbuf[w, :, at],
                (((1,), (1,)), ((), ())),
                preferred_element_type=jnp.float32,
            )
    inv = inverse(total)
    prods = [(prod * inv).astype(jnp.bfloat16).astype(jnp.float32) for prod in prods]

    for j in range(KV):
        asend[j] = jnp.concatenate(
            [prod[j * per : (j + 1) * per, :] for prod in prods], axis=0
        ).astype(jnp.bfloat16)
    for o in reversed(range(1, KV)):
        other = flip(kv, o)
        sent.append(push(1, asend.at[other], arecv.at[kv], o, other * TP + tp))
    arecv[kv] = asend[kv]
    for copy in small[2:]:
        copy.wait()
    for o in range(1, KV):
        other = flip(kv, o)
        take(1, asend.at[other], arecv.at[other], other * TP + tp)
    parts = [arecv[s].astype(jnp.float32) for s in range(KV)]
    for h in range(LH):
        row = jnp.concatenate([part[:, h * lc : (h + 1) * lc] for part in parts], axis=1)
        for i in range(4 * per):
            heads[i, h : h + 1, :] = row[i : i + 1, :]

    def kind(w):
        return heads[w * per : (w + 1) * per].reshape(per * LH, lane)

    low = jnp.concatenate([lb[...]] * per, axis=0)
    pre_q, pre_f, val, gate = kind(0), kind(1), kind(2), kind(3)
    forget = low + (1.0 - low) * sigmoid(pre_f)
    key = (1.0 - low) * sigmoid(-pre_f)
    query = pre_q * sigmoid(pre_q)
    items = per * LH
    stacked = jnp.concatenate(
        [forget, key, query, jnp.zeros((lane - 3 * items, lane), jnp.float32)], axis=0
    )
    cols = stacked.T
    state_in.wait()
    rows = []
    for i in range(items):
        new = (
            cols[:, i : i + 1] * stbuf[i]
            + cols[:, items + i : items + i + 1] * val[i : i + 1, :]
        )
        nsbuf[i] = new
        rows.append(
            jnp.sum(cols[:, 2 * items + i : 2 * items + i + 1] * new, axis=0, keepdims=True)
        )
    readout = jnp.concatenate(rows, axis=0)
    state_out = pltpu.make_async_copy(nsbuf, ns_h, local_sem.at[11])
    state_out.start()
    inv_head = lax.rsqrt(jnp.mean(readout * readout, axis=1, keepdims=True) + epsilon)
    gains = jnp.concatenate([hg[...]] * per, axis=0)
    mixed = readout * inv_head * gains * (gate * sigmoid(gate))
    for r in range(per):
        for h in range(LH):
            mrow[r : r + 1, h * lane : (h + 1) * lane] = mixed[r * LH + h : r * LH + h + 1, :]
    msend[...] = mrow[...].astype(jnp.bfloat16)
    spread(2, msend, mrecv)
    for o in range(1, N):
        take(2, msend, mrecv.at[order[o]], order[o])
    flat = jnp.concatenate(
        [
            jnp.concatenate(
                [mrecv[s * TP + t].astype(jnp.float32) for s in range(KV)], axis=0
            )
            for t in range(TP)
        ],
        axis=1,
    ).astype(jnp.bfloat16)

    out_in.wait()
    projected = jnp.dot(flat, obuf[...], preferred_element_type=jnp.float32)
    rsend[...] = (xsrc[...].astype(jnp.float32) + projected).astype(jnp.bfloat16)
    spread(3, rsend, rbuf)

    for copy in ups:
        copy.wait()
    tile = min(512, ubuf.shape[1])
    total = jnp.zeros((nb, 1), jnp.float32)
    for o in range(N):
        peer = order[o]
        if o:
            take(3, rsend, rbuf.at[peer], peer)
        at = columns(peer)
        piece, total = scaled(rbuf[peer], mlpg, at, total)
        for n in range(ubuf.shape[1] // tile):
            to = slice(n * tile, (n + 1) * tile)
            term = jnp.dot(piece, ubuf[at, to], preferred_element_type=jnp.float32)
            acc[:, to] = term if o == 0 else acc[:, to] + term
    act = jnp.maximum(acc[...] * inverse(total), 0.0)
    hid[...] = (act * act).astype(jnp.bfloat16)

    for copy in downs:
        copy.wait()

    def partial_sum(peer):
        return jnp.dot(hid[...], dbuf[:, columns(peer)], preferred_element_type=jnp.float32)

    for o in reversed(range(1, N)):
        psend[o] = partial_sum(order[o]).astype(jnp.bfloat16)
        sent.append(push(4, psend.at[o], pbuf.at[me], o, order[o]))
    summed = partial_sum(me)
    for o in range(1, N):
        take(4, psend.at[0], pbuf.at[order[o]], order[o])
        summed = summed + pbuf[order[o]].astype(jnp.float32)
    outbuf[...] = (rsend[...].astype(jnp.float32) + summed).astype(jnp.bfloat16)
    last = pltpu.make_async_copy(outbuf, out_h, local_sem.at[0])
    last.start()
    for copy in sent:
        copy.wait_send()
    last.wait()
    state_out.wait()


def local_kernel(KV, TP, *args):
    (tokens, mix_gain, qw, fw, vw, gw, lower_bound, state, head_gain, ow, mlp_gain, uw, dw) = args
    nb, block = tokens.shape
    LH, lc, D = qw.shape
    per, _, kd, vd = state.shape
    N = KV * TP
    UP, DOWN = 8, 8
    bf, f32 = jnp.bfloat16, jnp.float32
    flat = lambda a: a.reshape(-1, a.shape[-1])
    hidden = uw.shape[1]
    out, ns = pl.pallas_call(
        functools.partial(kernel, KV, TP, LH, UP, DOWN),
        out_shape=(
            jax.ShapeDtypeStruct((nb, block), bf),
            jax.ShapeDtypeStruct((per * LH, kd, vd), f32),
        ),
        in_specs=[pl.BlockSpec(memory_space=pl.ANY)] * 13,
        out_specs=(pl.BlockSpec(memory_space=pl.ANY),) * 2,
        scratch_shapes=[
            pltpu.VMEM((nb, block), bf),
            pltpu.VMEM((1, D), f32),
            pltpu.VMEM((LH, kd), f32),
            pltpu.VMEM((LH, vd), f32),
            pltpu.VMEM((1, D), f32),
            pltpu.VMEM((4, LH * lc, D), bf),
            pltpu.VMEM((per * LH, kd, vd), f32),
            pltpu.VMEM((per * LH, kd, vd), f32),
            pltpu.VMEM((ow.shape[0] * ow.shape[1], block), bf),
            pltpu.VMEM(uw.shape, bf),
            pltpu.VMEM(dw.shape, bf),
            pltpu.VMEM((nb, block), bf),
            pltpu.VMEM((N, nb, block), bf),
            pltpu.VMEM((KV, 4 * per, LH * lc), bf),
            pltpu.VMEM((KV, 4 * per, LH * lc), bf),
            pltpu.VMEM((4 * per, LH, kd), f32),
            pltpu.VMEM((per, LH * vd), f32),
            pltpu.VMEM((per, LH * vd), bf),
            pltpu.VMEM((N, per, LH * vd), bf),
            pltpu.VMEM((nb, block), bf),
            pltpu.VMEM((N, nb, block), bf),
            pltpu.VMEM((N, nb, block), bf),
            pltpu.VMEM((N, nb, block), bf),
            pltpu.VMEM((nb, hidden), f32),
            pltpu.VMEM((nb, hidden), bf),
            pltpu.SemaphoreType.DMA((12,)),
            pltpu.SemaphoreType.DMA((UP,)),
            pltpu.SemaphoreType.DMA((DOWN,)),
            pltpu.SemaphoreType.DMA((5, N)),
            pltpu.SemaphoreType.DMA((5, N)),
        ],
        compiler_params=pltpu.CompilerParams(
            collective_id=0, has_side_effects=True, vmem_limit_bytes=VMEM_LIMIT
        ),
    )(
        tokens, mix_gain.reshape(1, -1), flat(qw), flat(fw), flat(vw), flat(gw), lower_bound,
        state.reshape(-1, kd, vd), head_gain, flat(ow), mlp_gain.reshape(1, -1), uw, dw,
    )
    return out, ns.reshape(state.shape)


def local(KV, TP, *args):
    tokens, qw, state = args[0], args[2], args[7]
    nb, block = tokens.shape
    LH, lc, _ = qw.shape
    per, _, kd, vd = state.shape
    fits = (
        block % 128 == 0
        and (LH * lc) % 128 == 0
        and kd == 128
        and vd == 128
        and nb % 8 == 0
        and (4 * per) % 8 == 0
        and LH % 8 == 0
        and 3 * per * LH <= kd
        and args[11].shape[1] % 512 == 0
        and KV > 1
        and KV & (KV - 1) == 0
    )
    if fits:
        return local_kernel(KV, TP, *args)
    return local_plain(*args)


def solution(mesh):
    placed = (
        P("dp", ("kv", "tp")),
        P(),
        P("tp", "kv", None),
        P("tp", "kv", None),
        P("tp", "kv", None),
        P("tp", "kv", None),
        P("tp", None),
        P(("dp", "kv"), "tp", None, None),
        P("tp", None),
        P(None, None, ("kv", "tp")),
        P(),
        P(None, ("kv", "tp")),
        P(("kv", "tp"), None),
    )
    return jax.shard_map(
        functools.partial(local, mesh.shape["kv"], mesh.shape["tp"]),
        mesh=mesh,
        in_specs=placed,
        out_specs=(P("dp", ("kv", "tp")), P(("dp", "kv"), "tp", None, None)),
        check_vma=False,
    )
```
